32 devices in a mesh: sp: 4 (over z), fs: 4 (over y, x), tp: 2 (over core).
Axes of the slice: x: 2, y: 2, z: 4, core: 2. Of those that a mesh axis runs over, the one named last changes fastest.
Arguments:
- tokens: bfloat16 [4, 4096, 2048], P('fs', ('sp', 'tp')), may hold values from -6 to 6
- norm_gain: float32 [2048], replicated, may hold values from 0.1 to 1.9
- w_gate: bfloat16 [2048, 1024], P(('sp', 'fs'), 'tp'), may hold values from -0.125 to 0.125
- w_value: bfloat16 [2048, 1024], P(('sp', 'fs'), 'tp'), may hold values from -0.125 to 0.125
- w_bkey: bfloat16 [2048, 1024], P(('sp', 'fs'), 'tp'), may hold values from -0.125 to 0.125
- w_query: bfloat16 [2048, 1024], P(('sp', 'fs'), 'tp'), may hold values from -0.125 to 0.125
- w_pool_in: bfloat16 [2048, 1024], P(('sp', 'fs'), 'tp'), may hold values from -0.125 to 0.125
- w_step: bfloat16 [2048, 2, 16], replicated, may hold values from -0.125 to 0.125
- step_bias: float32 [2, 16], replicated, may hold values from -1 to 1
- decay_rate: float32 [2, 16], replicated, may hold values from 4.8828125e-06 to 0.06
- decay_shift: float32 [4, 16, 2, 4096], P('fs', 'tp', None, 'sp'), may hold values from 0 to 2.2
- conv_value: bfloat16 [5, 1024], replicated, may hold values from -2.5 to 2.5
- conv_bkey: bfloat16 [5, 1024], replicated, may hold values from -2.5 to 2.5
- conv_query: bfloat16 [5, 1024], replicated, may hold values from -2.5 to 2.5
- mix_gain: float32 [1024], replicated, may hold values from 0.1 to 1.9
- pool_mix: bfloat16 [8, 128, 128], replicated, may hold values from -0.5 to 0.5
- pool_gain: float32 [1024], replicated, may hold values from 0.1 to 1.9
- w_out_ssd: bfloat16 [1024, 2048], P('tp', ('sp', 'fs')), may hold values from -0.125 to 0.125
- w_out_pool: bfloat16 [1024, 2048], P('tp', ('sp', 'fs')), may hold values from -0.125 to 0.125
Outputs:
- mixed: bfloat16 [4, 4096, 2048], P('fs', ('sp', 'tp'))
The draws below stay inside these ranges and needn't reach their ends.
All inputs are finite; a program needn't handle non-finite values.
Results may differ from the reference program's by a relative error of at most 0.014.
Values may be sent and summed in bfloat16 or wider, within the bound.
A program may use at most 128 MiB of HBM per device.

```python
import jax
import jax.numpy as jnp
from jax import lax

D = 2048
HEAD_DIM = 64
DUALITY_HEADS = 16
GROUPS = 8
STATE = 128
CONV_WIDTH = 5
POOL_GROUPS = 8
POOL_DIM = 128
SPAN = 128
TOK_SP = 1024
SEQUENCE_LENGTH = 4096
BATCH_SEQUENCES = 4
D_SSM = 1024
D_POOL = 1024
N_TP = 2


def draw_decay_rate(key, part):
    order_key, slow_key, fast_key = jax.random.split(jax.random.fold_in(key, 11), 3)
    ranking = jax.random.permutation(order_key, 2 * DUALITY_HEADS)
    slow_count = DUALITY_HEADS
    slow_rate = jax.random.uniform(slow_key, (2 * DUALITY_HEADS,), jnp.float32, 0.02, 0.2) / SEQUENCE_LENGTH
    fast_rate = jax.random.uniform(fast_key, (2 * DUALITY_HEADS,), jnp.float32, 0.02, 0.06)
    rates = jnp.where(ranking < slow_count, slow_rate, fast_rate)
    return rates.reshape(2, DUALITY_HEADS).astype(jnp.float32)


def draw_decay_shift(key, part):
    random_keys = jax.random.split(jax.random.fold_in(key, 23), 4)
    token_position = jnp.arange(SEQUENCE_LENGTH, dtype=jnp.int32)
    segment = token_position // TOK_SP
    segments = SEQUENCE_LENGTH // TOK_SP
    low_end, high_end = (0.4, 2.5)
    factor = jnp.exp(jax.random.uniform(random_keys[0], (BATCH_SEQUENCES, DUALITY_HEADS, 2, segments), jnp.float32, jnp.log(low_end), jnp.log(high_end)))
    roughness = jax.random.uniform(random_keys[1], (BATCH_SEQUENCES, DUALITY_HEADS, 2, SEQUENCE_LENGTH), jnp.float32, 0.5, 1.5)
    reference_level = jnp.take(factor, segment, axis=3) * roughness * (0.3 / SEQUENCE_LENGTH)
    spike_places = jax.random.randint(random_keys[2], (BATCH_SEQUENCES, DUALITY_HEADS, 2, 3), 0, SEQUENCE_LENGTH)
    spike_length = jax.random.uniform(random_keys[3], (BATCH_SEQUENCES, DUALITY_HEADS, 2, 3), jnp.float32, 0.22, 0.69)
    match_count = (token_position[None, None, None, None, :] == spike_places[..., None]).astype(jnp.float32)
    spike_runs = jnp.sum(match_count * spike_length[..., None], axis=3)
    return (reference_level + spike_runs).astype(jnp.float32)


def levels(stream_key, shape, pieces, low, top_value):
    loudness = 1.0
    for dim, parts in pieces:
        steps = jax.random.uniform(jax.random.fold_in(jax.random.fold_in(stream_key, 6), dim), (parts,), jnp.float32, low / len(pieces), top_value / len(pieces))
        loudness = loudness * jnp.repeat(jnp.exp(steps), shape[dim] // parts).reshape((-1,) + (1,) * (len(shape) - 1 - dim))
    return loudness


def gaussian(own_key, extent, deviation, bound, cuts=(), held_as=jnp.bfloat16):
    array = deviation * jax.random.normal(own_key, extent, jnp.float32)
    if cuts:
        array = array * levels(own_key, extent, cuts, -0.22, 0.18)
    return jnp.clip(array, -bound, bound).astype(held_as)


def setup_inputs(seed: int = 0) -> dict:
    splits = jax.random.split(jax.random.key(seed), 20)
    tokens = gaussian(splits[0], (BATCH_SEQUENCES, SEQUENCE_LENGTH, D), 1.0, 6.0, ((0, 4), (1, 8)))
    norm_gain = jnp.clip(1.0 + 0.18 * jax.random.normal(splits[1], (D,), jnp.float32), 0.1, 1.9)
    w_gate = gaussian(splits[2], (D, D_SSM), D ** -0.5, 0.125, ((0, 16), (1, 2)))
    w_value = gaussian(splits[3], (D, D_SSM), D ** -0.5, 0.125, ((0, 16), (1, 2)))
    w_bkey = gaussian(splits[4], (D, GROUPS * STATE), D ** -0.5, 0.125, ((0, 16), (1, 2)))
    w_query = gaussian(splits[5], (D, GROUPS * STATE), D ** -0.5, 0.125, ((0, 16), (1, 2)))
    w_pool_in = gaussian(splits[6], (D, D_POOL), D ** -0.5, 0.125, ((0, 16), (1, 2)))
    w_step = gaussian(splits[7], (D, 2, DUALITY_HEADS), D ** -0.5, 0.125)
    step_bias = jnp.clip(jax.random.uniform(splits[8], (2, DUALITY_HEADS), jnp.float32, -1.0, 1.0), -1.0, 1.0)
    decay_rate = draw_decay_rate(jax.random.fold_in(splits[19], 71), 0)
    decay_shift = draw_decay_shift(jax.random.fold_in(splits[19], 71), 0)
    conv_value = gaussian(splits[11], (CONV_WIDTH, D_SSM), CONV_WIDTH ** -0.5, 2.5)
    conv_bkey = gaussian(splits[12], (CONV_WIDTH, GROUPS * STATE), CONV_WIDTH ** -0.5, 2.5)
    conv_query = gaussian(splits[13], (CONV_WIDTH, GROUPS * STATE), CONV_WIDTH ** -0.5, 2.5)
    mix_gain = jnp.clip(1.0 + 0.18 * jax.random.normal(splits[14], (D_SSM,), jnp.float32), 0.1, 1.9)
    pool_mix = gaussian(splits[15], (POOL_GROUPS, POOL_DIM, POOL_DIM), POOL_DIM ** -0.5, 0.5)
    pool_gain = jnp.clip(1.0 + 0.18 * jax.random.normal(splits[16], (D_POOL,), jnp.float32), 0.1, 1.9)
    w_out_ssd = gaussian(splits[17], (D_SSM, D), (D_SSM + D_POOL) ** -0.5, 0.125, ((0, 2), (1, 16)))
    w_out_pool = gaussian(splits[18], (D_POOL, D), (D_SSM + D_POOL) ** -0.5, 0.125, ((0, 2), (1, 16)))
    return {"tokens": tokens, "norm_gain": norm_gain, "w_gate": w_gate, "w_value": w_value, "w_bkey": w_bkey, "w_query": w_query, "w_pool_in": w_pool_in, "w_step": w_step, "step_bias": step_bias, "decay_rate": decay_rate, "decay_shift": decay_shift, "conv_value": conv_value, "conv_bkey": conv_bkey, "conv_query": conv_query, "mix_gain": mix_gain, "pool_mix": pool_mix, "pool_gain": pool_gain, "w_out_ssd": w_out_ssd, "w_out_pool": w_out_pool}


EPSILON = 1e-06
HIGHEST = lax.Precision.HIGHEST
WINDOWS = (2, 4, 8, 16)

def blockwise(values, bkeys, queries, steps, logs):
    length, heads, head_width = values.shape
    groups, state_width = (bkeys.shape[1], bkeys.shape[2])
    per_group = heads // groups
    blocks = length // SPAN
    weighted = (values * jnp.transpose(steps)[:, :, None]).reshape(blocks, SPAN, groups, per_group, head_width)
    key_blocks = bkeys.reshape(blocks, SPAN, groups, state_width)
    query_blocks = queries.reshape(blocks, SPAN, groups, state_width)
    inner = jnp.cumsum(logs.reshape(heads, blocks, SPAN), axis=-1)
    lower = jnp.tril(jnp.ones((SPAN, SPAN), dtype=bool))
    within = jnp.exp(jnp.where(lower, inner[..., :, None] - inner[..., None, :], -jnp.inf))
    within = within.reshape(groups, per_group, blocks, SPAN, SPAN)
    scores = jnp.einsum('clgn,csgn->cgls', query_blocks, key_blocks, precision=HIGHEST)
    diagonal = jnp.einsum('cgls,gkcls,csgkp->clgkp', scores, within, weighted, precision=HIGHEST)
    tails = jnp.exp(inner[..., -1:] - inner).reshape(groups, per_group, blocks, SPAN)
    ends = jnp.einsum('clgn,gkcl,clgkp->cgkpn', key_blocks, tails, weighted, precision=HIGHEST)
    totals = inner[..., -1]
    upto = jnp.cumsum(totals, axis=-1)
    before = upto - totals
    block_ids = jnp.arange(blocks, dtype=jnp.int32)
    earlier = block_ids[None, :] < block_ids[:, None]
    between = jnp.exp(jnp.where(earlier[None], before[:, :, None] - upto[:, None, :], -jnp.inf))
    between = between.reshape(groups, per_group, blocks, blocks)
    prior = jnp.einsum('gkcj,jgkpn->cgkpn', between, ends, precision=HIGHEST)
    reach = jnp.exp(inner).reshape(groups, per_group, blocks, SPAN)
    offdiag = jnp.einsum('clgn,cgkpn,gkcl->clgkp', query_blocks, prior, reach, precision=HIGHEST)
    return (diagonal + offdiag).reshape(length, heads, head_width)

def centred(projected, taps):
    margin = CONV_WIDTH // 2
    length = projected.shape[0]
    padded = jnp.pad(projected, ((margin, margin), (0, 0)))
    running = jnp.zeros(projected.shape, jnp.float32)
    for offset in range(CONV_WIDTH):
        running = running + padded[offset:offset + length].astype(jnp.float32) * taps[offset].astype(jnp.float32)
    return running

def box_mean(column, window):
    length = column.shape[0]
    prefix = jnp.pad(jnp.cumsum(column, axis=0), ((1, 0), (0, 0)))
    where_now = jnp.arange(length, dtype=jnp.int32)
    lower = jnp.clip(where_now - window // 2, 0, length).astype(jnp.int32)
    upper = jnp.clip(where_now + window - window // 2, 0, length).astype(jnp.int32)
    counts = (upper - lower).astype(jnp.float32)
    return (prefix[upper] - prefix[lower]) / counts[:, None]

def reference(tokens, norm_gain, w_gate, w_value, w_bkey, w_query, w_pool_in, w_step, step_bias, decay_rate, decay_shift, conv_value, conv_bkey, conv_query, mix_gain, pool_mix, pool_gain, w_out_ssd, w_out_pool):

    def one_sequence(paired):
        rows, shift = paired
        length = rows.shape[0]
        widened = rows.astype(jnp.float32)
        normed = (widened * lax.rsqrt(lax.optimization_barrier(jnp.mean(widened * widened, axis=-1, keepdims=True)) + EPSILON) * norm_gain).astype(jnp.bfloat16)
        gate = jnp.dot(normed, w_gate, preferred_element_type=jnp.float32).astype(jnp.bfloat16)
        value = jnp.dot(normed, w_value, preferred_element_type=jnp.float32).astype(jnp.bfloat16)
        bkey = jnp.dot(normed, w_bkey, preferred_element_type=jnp.float32).astype(jnp.bfloat16)
        query = jnp.dot(normed, w_query, preferred_element_type=jnp.float32).astype(jnp.bfloat16)
        pooled = jnp.dot(normed, w_pool_in, preferred_element_type=jnp.float32).astype(jnp.bfloat16)
        raw_steps = jnp.dot(normed, w_step.reshape(D, 2 * DUALITY_HEADS), preferred_element_type=jnp.float32)
        steps = jax.nn.softplus(raw_steps.reshape(length, 2, DUALITY_HEADS) + step_bias).transpose(1, 2, 0)
        logs = -decay_rate[:, :, None] * steps - shift.transpose(1, 0, 2)
        values = jax.nn.silu(centred(value, conv_value)).reshape(length, DUALITY_HEADS, HEAD_DIM)
        bkeys = jax.nn.silu(centred(bkey, conv_bkey)).reshape(length, GROUPS, STATE)
        queries = jax.nn.silu(centred(query, conv_query)).reshape(length, GROUPS, STATE)
        forward = blockwise(values, bkeys, queries, steps[0], logs[0])
        backward = blockwise(values[::-1], bkeys[::-1], queries[::-1], steps[1][:, ::-1], logs[1][:, ::-1])[::-1]
        heads_out = forward + backward
        gated = heads_out.reshape(length, D_SSM) * jax.nn.silu(gate.astype(jnp.float32))
        ssd_mix = (gated * lax.rsqrt(lax.optimization_barrier(jnp.mean(gated * gated, axis=-1, keepdims=True)) + EPSILON) * mix_gain).astype(jnp.bfloat16)
        pool_rows = pooled.astype(jnp.float32).reshape(length, POOL_GROUPS, POOL_DIM)
        differences = []
        for group in range(POOL_GROUPS):
            column = pool_rows[:, group]
            differences.append(box_mean(column, WINDOWS[group % 4]) - column)
        pool_diff = jnp.stack(differences, axis=1).astype(jnp.bfloat16)
        mapped = jnp.einsum('sgc,gcd->sgd', pool_diff.astype(jnp.float32), pool_mix.astype(jnp.float32))
        pool_out = (mapped.reshape(length, D_POOL) * pool_gain).astype(jnp.bfloat16)
        ssd_part = D_SSM // N_TP
        pool_part = D_POOL // N_TP
        summed = jnp.zeros((length, D), jnp.float32)
        for member in range(N_TP):
            partial_value = jnp.dot(ssd_mix[:, member * ssd_part:(member + 1) * ssd_part], w_out_ssd[member * ssd_part:(member + 1) * ssd_part], preferred_element_type=jnp.float32)
            partial_value = partial_value + jnp.dot(pool_out[:, member * pool_part:(member + 1) * pool_part], w_out_pool[member * pool_part:(member + 1) * pool_part], preferred_element_type=jnp.float32)
            rounded = lax.optimization_barrier(partial_value.astype(jnp.bfloat16))
            summed = summed + rounded.astype(jnp.float32)
        return summed.astype(jnp.bfloat16)
    return lax.map(one_sequence, (tokens, decay_shift))
```

```python
import functools

import jax
import jax.numpy as jnp
from jax import lax
from jax.experimental import pallas as pl
from jax.experimental.pallas import tpu as pltpu
from jax.sharding import PartitionSpec as P

HEAD_DIM = 64
DUALITY_HEADS = 16
GROUPS = 8
STATE = 128
CONV_WIDTH = 5
POOL_GROUPS = 8
POOL_DIM = 128
SPAN = 128
REACH = 8
D_SSM = 1024


EPSILON = 1e-06
HIGHEST = lax.Precision.HIGHEST
WINDOWS = (2, 4, 8, 16)


def padded_2(cells, sides, width):
    for axis, dim in sides:
        count = lax.axis_size(axis)
        ends = count - 1
        head = lax.slice_in_dim(cells, 0, width, axis=dim)
        tail = lax.slice_in_dim(cells, cells.shape[dim] - width, cells.shape[dim], axis=dim)
        cells = jnp.concatenate(
            [
                lax.ppermute(tail, axis, [(i, (i + 1) % count) for i in range(ends)]),
                cells,
                lax.ppermute(head, axis, [((i + 1) % count, i) for i in range(ends)]),
            ],
            axis=dim,
        )
    return cells


MESH = pl.DeviceIdType.MESH


def gather_kernel(n_sp, n_tp, w_ref, t_ref, w_out, t_out, send, recv, local_sem):
    z = lax.axis_index("sp")
    f = lax.axis_index("fs")
    c = lax.axis_index("tp")
    fx = f + 1 - 2 * lax.rem(f, 2)
    fy = lax.rem(f + 2, 4)
    rows = w_ref.shape[0]
    half = rows // 2
    x_dev = (z, fx, c)
    y_dev = (z, fy, c)
    z_devs = [(lax.rem(z + d, n_sp), f, c) for d in range(1, n_sp)]
    t_devs = [(z, f, lax.rem(c + d, n_tp)) for d in range(1, n_tp)]
    partners = [x_dev, y_dev] + z_devs + t_devs
    barrier = pltpu.get_barrier_semaphore()
    for dev in partners:
        pl.semaphore_signal(barrier, inc=1, device_id=dev, device_id_type=MESH)
    pl.semaphore_wait(barrier, len(partners))

    def remote(src, dst, index, dev):
        copy = pltpu.make_async_remote_copy(
            src_ref=src,
            dst_ref=dst,
            send_sem=send.at[index],
            recv_sem=recv.at[index],
            device_id=dev,
            device_id_type=MESH,
        )
        copy.start()
        return copy

    base = n_sp - 1
    z_copies = [remote(w_ref, w_out.at[z, f], d, z_devs[d]) for d in range(n_sp - 1)]
    full = []
    relay = []

    def send_full(d):
        if d == 0:
            src = w_ref
            origin = z
        else:
            z_copies[d - 1].wait_recv()
            origin = lax.rem(z - d + n_sp, n_sp)
            src = w_out.at[origin, f]
        dst = w_out.at[origin, f]
        full.append(
            (
                remote(src, dst, base + 4 * d, x_dev),
                remote(src, dst, base + 4 * d + 1, y_dev),
            )
        )

    def send_relay(d):
        origin = lax.rem(z - d + n_sp, n_sp)
        full[d][0].wait_recv()
        part = w_out.at[origin, fx, pl.ds(0, half)]
        first = remote(part, part, base + 4 * d + 2, y_dev)
        full[d][1].wait_recv()
        part = w_out.at[origin, fy, pl.ds(half, half)]
        relay.append((first, remote(part, part, base + 4 * d + 3, x_dev)))

    send_full(0)
    own_w = pltpu.make_async_copy(w_ref, w_out.at[z, f], local_sem.at[0])
    own_w.start()
    own_t = pltpu.make_async_copy(t_ref, t_out.at[c], local_sem.at[1])
    own_t.start()
    tbase = base + 4 * n_sp
    t_copies = [remote(t_ref, t_out.at[c], tbase + d, t_devs[d]) for d in range(n_tp - 1)]
    for d in range(1, n_sp):
        send_full(d)
        send_relay(d - 1)
    send_relay(n_sp - 1)
    for pair in relay:
        for copy in pair:
            copy.wait_recv()
    for copy in t_copies:
        copy.wait_recv()
    for copy in z_copies + t_copies:
        copy.wait_send()
    for pair in full + relay:
        for copy in pair:
            copy.wait_send()
    own_w.wait()
    own_t.wait()


def gather_inputs(weights, tokens):
    n_sp = lax.axis_size("sp")
    n_fs = lax.axis_size("fs")
    n_tp = lax.axis_size("tp")
    rows, cols = weights.shape
    if n_fs != 4:
        return (
            lax.all_gather(weights, ("sp", "fs"), axis=0, tiled=True),
            lax.all_gather(tokens, "tp", axis=0, tiled=True),
        )
    count = (n_sp - 1) + 4 * n_sp + (n_tp - 1)
    wide, toks = pl.pallas_call(
        functools.partial(gather_kernel, n_sp, n_tp),
        out_shape=(
            jax.ShapeDtypeStruct((n_sp, n_fs, rows, cols), weights.dtype),
            jax.ShapeDtypeStruct((n_tp,) + tokens.shape, tokens.dtype),
        ),
        in_specs=[pl.BlockSpec(memory_space=pltpu.VMEM)] * 2,
        out_specs=[pl.BlockSpec(memory_space=pl.ANY)] * 2,
        scratch_shapes=[
            pltpu.SemaphoreType.DMA((count,)),
            pltpu.SemaphoreType.DMA((count,)),
            pltpu.SemaphoreType.DMA((2,)),
        ],
        compiler_params=pltpu.CompilerParams(collective_id=0, has_side_effects=True),
        cost_estimate=pl.CostEstimate(
            flops=0, bytes_accessed=200 * n_sp * n_fs * rows * cols, transcendentals=0
        ),
        name="gather_inputs",
    )(weights, tokens)
    return wide.reshape(n_sp * n_fs * rows, cols), toks.reshape(-1, tokens.shape[1])


def split_heads(first, second, axis, shape):
    places = lax.broadcasted_iota(jnp.int32, shape, axis)
    return jnp.where(places < HEAD_DIM, first, second)


def ends_kernel(blocks, decay_ref, x_ref, k_ref, col_ref, ends_ref, final_ref):
    group = pl.program_id(0)
    tile = (SPAN, 2 * HEAD_DIM)
    for c in range(blocks):
        rows = pl.ds(c * SPAN, SPAN)
        x = x_ref[rows, :].astype(jnp.float32)
        k = k_ref[rows, :]
        for r in range(2):
            weight = split_heads(
                col_ref[0, rows, 4 + 2 * r : 5 + 2 * r],
                col_ref[0, rows, 5 + 2 * r : 6 + 2 * r],
                1,
                tile,
            )
            end = lax.dot_general(
                (x * weight).astype(jnp.bfloat16),
                k,
                (((0,), (0,)), ((), ())),
                preferred_element_type=jnp.float32,
            )
            ends_ref[0, r, c] = end
    states = (2 * HEAD_DIM, STATE)
    for r in range(2):
        total = jnp.zeros(states, jnp.float32)
        for c in range(blocks) if r == 0 else range(blocks - 1, -1, -1):
            at = ((group * blocks + c) * 2 + r) * 2
            scale = split_heads(decay_ref[at], decay_ref[at + 1], 0, states)
            total = total * scale + ends_ref[0, r, c]
        final_ref[0, r] = total


def outputs_kernel(
    blocks, decay_ref, x_ref, k_ref, q_ref, col_ref, row_ref, ends_ref, in_ref, y_ref, prior
):
    group = pl.program_id(0)
    states = (2 * HEAD_DIM, STATE)
    tile = (SPAN, 2 * HEAD_DIM)
    square = (SPAN, SPAN)
    for r in range(2):
        total = in_ref[0, r]
        for c in range(blocks) if r == 0 else range(blocks - 1, -1, -1):
            prior[r, c] = total.astype(jnp.bfloat16)
            at = ((group * blocks + c) * 2 + r) * 2
            scale = split_heads(decay_ref[at], decay_ref[at + 1], 0, states)
            total = total * scale + ends_ref[0, r, c]
    later = lax.broadcasted_iota(jnp.int32, square, 0)
    sooner = lax.broadcasted_iota(jnp.int32, square, 1)
    lower = later >= sooner
    equal = later == sooner
    across = (((1,), (1,)), ((), ()))
    for c in range(blocks):
        rows = pl.ds(c * SPAN, SPAN)
        x = x_ref[rows, :]
        q = q_ref[rows, :]
        scores = lax.dot_general(q, k_ref[rows, :], across, preferred_element_type=jnp.float32)
        parts = []
        for h in range(2):
            cf_l = col_ref[0, rows, 2 * h : 2 * h + 1]
            eb_l = col_ref[0, rows, 2 * h + 1 : 2 * h + 2]
            cf_s = row_ref[0, 4 * h : 4 * h + 1, rows]
            eb_s = row_ref[0, 4 * h + 1 : 4 * h + 2, rows]
            df_s = row_ref[0, 4 * h + 2 : 4 * h + 3, rows]
            db_s = row_ref[0, 4 * h + 3 : 4 * h + 4, rows]
            decay = jnp.exp(jnp.where(lower, cf_l - cf_s, eb_s - eb_l))
            step = jnp.where(equal, df_s + db_s, jnp.where(lower, df_s, db_s))
            parts.append(
                jnp.dot(
                    (scores * decay * step).astype(jnp.bfloat16),
                    x,
                    preferred_element_type=jnp.float32,
                )
            )
        out = split_heads(parts[0], parts[1], 1, tile)
        for r in range(2):
            reach = split_heads(
                col_ref[0, rows, 8 + 2 * r : 9 + 2 * r],
                col_ref[0, rows, 9 + 2 * r : 10 + 2 * r],
                1,
                tile,
            )
            out = out + reach * lax.dot_general(
                q, prior[r, c], across, preferred_element_type=jnp.float32
            )
        y_ref[rows, :] = out


def mixer(activated, width_ssd, width_key, steps, logs, sp_rank):
    length = activated.shape[0]
    heads = steps.shape[1]
    groups = width_key // STATE
    blocks = length // SPAN
    shaped = logs.reshape(2, heads, blocks, SPAN)
    ones = jnp.triu(jnp.ones((SPAN, SPAN), jnp.float32))
    inner = jnp.einsum("rhcs,sl->rhcl", shaped, ones, precision=HIGHEST)
    totals = inner[..., -1:]
    cf = inner[0]
    eb = inner[1] - shaped[1]
    wf = jnp.exp(totals[0] - cf) * steps[0].reshape(cf.shape)
    wb = jnp.exp(eb) * steps[1].reshape(cf.shape)
    reach_f = jnp.exp(cf)
    reach_b = jnp.exp(totals[1] - eb)

    def pair(a):
        return a.reshape(groups, 2, length)

    cf, eb, wf, wb, reach_f, reach_b = map(pair, (cf, eb, wf, wb, reach_f, reach_b))
    df, db = (pair(steps[0]), pair(steps[1]))
    packed = jnp.stack(
        [cf[:, 0], eb[:, 0], cf[:, 1], eb[:, 1]]
        + [wf[:, 0], wf[:, 1], wb[:, 0], wb[:, 1]]
        + [reach_f[:, 0], reach_f[:, 1], reach_b[:, 0], reach_b[:, 1]],
        axis=1,
    )
    cols = jnp.transpose(packed, (0, 2, 1))
    rows = jnp.stack(
        [cf[:, 0], eb[:, 0], df[:, 0], db[:, 0], cf[:, 1], eb[:, 1], df[:, 1], db[:, 1]], axis=1
    )
    block_logs = totals[..., 0]
    decays = jnp.exp(block_logs).reshape(2, groups, 2, blocks)
    decays = jnp.transpose(decays, (1, 3, 0, 2)).reshape(-1)
    smem = pl.BlockSpec(memory_space=pltpu.SMEM)
    x_blocks = width_ssd // STATE

    def wide(offset):
        return pl.BlockSpec((length, STATE), lambda g: (0, g + offset))

    col_spec = pl.BlockSpec((1, length, cols.shape[2]), lambda g: (g, 0, 0))
    ends_spec = pl.BlockSpec((1, 2, blocks, STATE, STATE), lambda g: (g, 0, 0, 0, 0))
    state_spec = pl.BlockSpec((1, 2, STATE, STATE), lambda g: (g, 0, 0, 0))
    ends, finals = pl.pallas_call(
        functools.partial(ends_kernel, blocks),
        grid=(groups,),
        out_shape=(
            jax.ShapeDtypeStruct((groups, 2, blocks, STATE, STATE), jnp.float32),
            jax.ShapeDtypeStruct((groups, 2, STATE, STATE), jnp.float32),
        ),
        in_specs=[smem, wide(0), wide(x_blocks), col_spec],
        out_specs=(ends_spec, state_spec),
        cost_estimate=pl.CostEstimate(
            flops=4 * length * groups * STATE * STATE,
            bytes_accessed=16 * length * groups * STATE,
            transcendentals=0,
        ),
        name="block_ends",
    )(decays, activated, activated, cols)
    device_totals = jnp.sum(block_logs, axis=-1)
    all_totals = lax.all_gather(
        device_totals[None].astype(jnp.bfloat16), "sp", axis=0, tiled=True
    ).astype(jnp.float32)
    states = jnp.transpose(finals, (1, 0, 2, 3)).reshape(2, heads, HEAD_DIM, STATE)
    forward_in, backward_in = prefix_states(all_totals, states.astype(jnp.bfloat16), sp_rank)
    incoming = jnp.stack([forward_in, backward_in]).reshape(2, groups, STATE, STATE)
    incoming = jnp.transpose(incoming, (1, 0, 2, 3))
    return pl.pallas_call(
        functools.partial(outputs_kernel, blocks),
        grid=(groups,),
        out_shape=jax.ShapeDtypeStruct((length, groups * STATE), jnp.float32),
        in_specs=[
            smem,
            wide(0),
            wide(x_blocks),
            wide(x_blocks + groups),
            col_spec,
            pl.BlockSpec((1, 8, length), lambda g: (g, 0, 0)),
            ends_spec,
            state_spec,
        ],
        out_specs=wide(0),
        scratch_shapes=[pltpu.VMEM((2, blocks, STATE, STATE), jnp.bfloat16)],
        cost_estimate=pl.CostEstimate(
            flops=10 * length * groups * STATE * STATE,
            bytes_accessed=40 * length * groups * STATE,
            transcendentals=2 * length * groups * SPAN,
        ),
        name="block_outputs",
    )(decays, activated, activated, activated, cols, rows, ends, incoming)


def prefix_states(all_totals, finals, rank):
    chain_length = all_totals.shape[0]
    device_ids = jnp.arange(chain_length, dtype=jnp.int32)[:, None]
    forward_cum = jnp.cumsum(all_totals[:, 0], axis=0)
    forward_mine = lax.dynamic_slice_in_dim(forward_cum - all_totals[:, 0], rank, 1, 0)
    forward_weight = jnp.exp(jnp.where(device_ids < rank, forward_mine - forward_cum, -jnp.inf))
    backward_cum = jnp.cumsum(all_totals[:, 1], axis=0)
    backward_mine = lax.dynamic_slice_in_dim(backward_cum, rank, 1, 0)
    backward_weight = jnp.exp(
        jnp.where(device_ids > rank, backward_cum - all_totals[:, 1] - backward_mine, -jnp.inf)
    )
    forward_in = jnp.zeros(finals.shape[1:], jnp.float32)
    backward_in = jnp.zeros(finals.shape[1:], jnp.float32)
    for d in range(1, chain_length):
        ahead = [(i, i + d) for i in range(chain_length - d)]
        back = [(i + d, i) for i in range(chain_length - d)]
        from_left = lax.ppermute(finals[0], "sp", ahead).astype(jnp.float32)
        from_right = lax.ppermute(finals[1], "sp", back).astype(jnp.float32)
        left = lax.dynamic_index_in_dim(forward_weight, jnp.maximum(rank - d, 0), 0, False)
        right = lax.dynamic_index_in_dim(
            backward_weight, jnp.minimum(rank + d, chain_length - 1), 0, False
        )
        forward_in = forward_in + left[:, None, None] * from_left
        backward_in = backward_in + right[:, None, None] * from_right
    return (forward_in, backward_in)


def local(
    tokens,
    norm_gain,
    w_gate,
    w_value,
    w_bkey,
    w_query,
    w_pool_in,
    w_step,
    step_bias,
    decay_rate,
    decay_shift,
    conv_value,
    conv_bkey,
    conv_query,
    mix_gain,
    pool_mix,
    pool_gain,
    w_out_ssd,
    w_out_pool,
):
    tp_count = lax.axis_size("tp")
    sp_count = lax.axis_size("sp")
    tp_rank = lax.axis_index("tp")
    sp_rank = lax.axis_index("sp")
    heads_dev = DUALITY_HEADS // tp_count
    groups_dev = GROUPS // tp_count
    pools_dev = POOL_GROUPS // tp_count
    width_ssd = heads_dev * HEAD_DIM
    width_key = groups_dev * STATE
    width_pool = pools_dev * POOL_DIM
    weights = jnp.concatenate([w_gate, w_value, w_bkey, w_query, w_pool_in], axis=1)
    combined, widened = gather_inputs(weights, tokens[0])
    out_rows = lax.all_gather(
        jnp.concatenate([w_out_ssd, w_out_pool], axis=0), ("sp", "fs"), axis=1, tiled=True
    )
    step_cols = lax.dynamic_slice_in_dim(w_step, tp_rank * heads_dev, heads_dev, 2)
    step_cols = step_cols.reshape(w_step.shape[0], 2 * heads_dev)
    widened = widened.astype(jnp.float32)
    scaling = lax.rsqrt(jnp.mean(widened * widened, axis=-1, keepdims=True) + EPSILON)
    normed = (widened * scaling * norm_gain).astype(jnp.bfloat16)
    stored = jnp.dot(normed, combined, preferred_element_type=jnp.float32).astype(jnp.bfloat16)
    raw_steps = jnp.dot(normed, step_cols, preferred_element_type=jnp.float32)
    length = stored.shape[0]
    padded = padded_2(stored[:, width_ssd:], (("sp", 0),), REACH)
    conv_cols = width_ssd + 2 * width_key
    taps = jnp.concatenate(
        [
            lax.dynamic_slice_in_dim(conv_value, tp_rank * width_ssd, width_ssd, 1),
            lax.dynamic_slice_in_dim(conv_bkey, tp_rank * width_key, width_key, 1),
            lax.dynamic_slice_in_dim(conv_query, tp_rank * width_key, width_key, 1),
        ],
        axis=1,
    ).astype(jnp.float32)
    margin = CONV_WIDTH // 2
    convolved = jnp.zeros((length, conv_cols), jnp.float32)
    for offset in range(CONV_WIDTH):
        begin = REACH - margin + offset
        convolved = (
            convolved
            + padded[begin : begin + length, :conv_cols].astype(jnp.float32) * taps[offset]
        )
    activated = jax.nn.silu(convolved).astype(jnp.bfloat16)
    bias_dev = lax.dynamic_slice_in_dim(step_bias, tp_rank * heads_dev, heads_dev, 1)
    rate_dev = lax.dynamic_slice_in_dim(decay_rate, tp_rank * heads_dev, heads_dev, 1)
    steps = jax.nn.softplus(raw_steps.reshape(length, 2, heads_dev) + bias_dev).transpose(1, 2, 0)
    logs = -rate_dev[:, :, None] * steps - decay_shift[0].transpose(1, 0, 2)
    heads_out = mixer(activated, width_ssd, width_key, steps, logs, sp_rank)
    gated = heads_out * jax.nn.silu(stored[:, :width_ssd].astype(jnp.float32))
    squares = lax.psum(jnp.sum(gated * gated, axis=-1), "tp")
    gain_dev = lax.dynamic_slice_in_dim(mix_gain, tp_rank * width_ssd, width_ssd, 0)
    ssd_mix = (gated * lax.rsqrt(squares / D_SSM + EPSILON)[:, None] * gain_dev).astype(
        jnp.bfloat16
    )
    pool_rows = padded[:, conv_cols:].astype(jnp.float32)
    own_rows = pool_rows[REACH : REACH + length]
    where_global = sp_rank * length + jnp.arange(length, dtype=jnp.int32)
    seq_length = length * sp_count
    window_means = []
    for window in WINDOWS:
        running = jnp.zeros((length, width_pool), jnp.float32)
        for offset in range(-(window // 2), window - window // 2):
            running = running + pool_rows[REACH + offset : REACH + offset + length]
        lower = jnp.clip(where_global - window // 2, 0, seq_length)
        upper = jnp.clip(where_global + window - window // 2, 0, seq_length)
        window_means.append(running / (upper - lower).astype(jnp.float32)[:, None])
    stacked = jnp.stack(window_means).reshape(4, length, pools_dev, POOL_DIM)
    group_ids = tp_rank * pools_dev + jnp.arange(pools_dev, dtype=jnp.int32)
    selector = (jnp.arange(4, dtype=jnp.int32)[:, None] == (group_ids % 4)[None, :]).astype(
        jnp.float32
    )
    means = jnp.sum(stacked * selector[:, None, :, None], axis=0)
    differences = (means - own_rows.reshape(length, pools_dev, POOL_DIM)).astype(jnp.bfloat16)
    pool_weights = lax.dynamic_slice_in_dim(pool_mix, tp_rank * pools_dev, pools_dev, 0)
    mapped = jnp.einsum(
        "rgc,gcd->rgd", differences, pool_weights, preferred_element_type=jnp.float32
    )
    pool_gain_dev = lax.dynamic_slice_in_dim(pool_gain, tp_rank * width_pool, width_pool, 0)
    pool_out = (mapped.reshape(length, width_pool) * pool_gain_dev).astype(jnp.bfloat16)
    mixed = jnp.concatenate([ssd_mix, pool_out], axis=1)
    if tp_count == 2:
        part = length // 2
        away = lax.dynamic_slice_in_dim(mixed, (1 - tp_rank) * part, part, 0)
        home = lax.dynamic_slice_in_dim(mixed, tp_rank * part, part, 0)
        sent = jnp.dot(away, out_rows, preferred_element_type=jnp.float32).astype(jnp.bfloat16)
        received = lax.ppermute(sent, "tp", [(0, 1), (1, 0)])
        kept = lax.optimization_barrier(
            jnp.dot(home, out_rows, preferred_element_type=jnp.float32).astype(jnp.bfloat16)
        )
        summed = (kept.astype(jnp.float32) + received.astype(jnp.float32)).astype(jnp.bfloat16)
    else:
        summed = lax.psum_scatter(
            jnp.dot(mixed, out_rows, preferred_element_type=jnp.float32).astype(jnp.bfloat16),
            "tp",
            scatter_dimension=0,
            tiled=True,
        )
    return summed[None]


def solution(mesh):
    return jax.shard_map(
        local,
        mesh=mesh,
        in_specs=(
            P("fs", ("sp", "tp"), None),
            P(),
            P(("sp", "fs"), "tp"),
            P(("sp", "fs"), "tp"),
            P(("sp", "fs"), "tp"),
            P(("sp", "fs"), "tp"),
            P(("sp", "fs"), "tp"),
            P(),
            P(),
            P(),
            P("fs", "tp", None, "sp"),
            P(),
            P(),
            P(),
            P(),
            P(),
            P(),
            P("tp", ("sp", "fs")),
            P("tp", ("sp", "fs")),
        ),
        out_specs=P("fs", ("sp", "tp"), None),
        check_vma=False,
    )
```
